32 devices in a mesh: sp: 8 (over z, y), tp: 4 (over x, core).
Axes of the slice: x: 2, y: 2, z: 4, core: 2. Of those that a mesh axis runs over, the one named last changes fastest.
Arguments:
- query_rows: bfloat16 [2560, 1024], P('sp', 'tp'), may hold values from -6 to 6
- key_rows: bfloat16 [2560, 1024], P('sp', 'tp'), may hold values from -6 to 6
- value_rows: bfloat16 [2560, 1024], P('sp', 'tp'), may hold values from -6 to 6
- key_shift: bfloat16 [2560, 16], P('sp', 'tp'), may hold values from -10 to 6
- documents: int32 [2560], P('sp'), may hold values from 0 to 3, never falling along the last dimension, each value on 1 to 1280 neighbouring positions
- out_weight: bfloat16 [1024, 2048], P('tp'), may hold values from -0.1875 to 0.1875
- stream: bfloat16 [2560, 2048], P('sp', 'tp'), may hold values from -8 to 8
- norm_gain: float32 [2048], replicated, may hold values from 0.1 to 1.9
- expert_ids: int32 [2560, 2], P('sp'), may hold values from 0 to 7, all different within a row; in each aligned block of 320 rows (0 to 319, 320 to 639, ...) at most 107 rows name the same one
- expert_weights: float32 [2560, 2], P('sp'), may hold values from 0.25 to 1
- gate_weight: bfloat16 [8, 2048, 3584], P('sp', None, 'tp'), may hold values from -0.125 to 0.125
- up_weight: bfloat16 [8, 2048, 3584], P('sp', None, 'tp'), may hold values from -0.125 to 0.125
- down_weight: bfloat16 [8, 3584, 2048], P('sp', 'tp'), may hold values from -0.09375 to 0.09375
Outputs:
- layer_out: bfloat16 [2560, 2048], P('sp', 'tp')
The draws below stay inside these ranges and needn't reach their ends.
Inputs may be any that keep to these rules, and one draw needn't show every extreme that they name: `expert_ids`: in each aligned block of 320 rows no expert is named by more than 107 rows, a bound that some block reaches; the entries of a row differ. `documents`: document numbers never fall along the positions; each document has 1 to 1280 positions, and one has exactly 1280.
All inputs are finite; a program needn't handle non-finite values.
Results may differ from the reference program's by a relative error of at most 0.013.
Values may be sent and summed in bfloat16 or wider, within the bound.
A program may use at most 128 MiB of HBM per device.

```python
import math
import jax
import jax.numpy as jnp
import numpy as np
from jax import lax

D = 2048
HEADS = 16
HEAD = 64
FF = 3584
TOP_K = 2
REACH = 4
SHARD = 320
PACKED_TOKENS = 2560
EXPERTS = 8
CAP = 107
DOC_MOST = 1280
DOCS = 4
N_SP = 8
N_TP = 4


def draw_value_rows(key, part):
    noise_key, offset_key = jax.random.split(key)
    row_width = HEADS * HEAD
    noise_part = jax.random.normal(noise_key, (PACKED_TOKENS, row_width), jnp.float32)
    offset = jax.random.uniform(offset_key, (PACKED_TOKENS // SHARD, 1, row_width), jnp.float32, -1.5, 1.5)
    shifted = noise_part.reshape(PACKED_TOKENS // SHARD, SHARD, row_width) + offset
    return jnp.clip(shifted.reshape(PACKED_TOKENS, row_width), -6.0, 6.0).astype(jnp.bfloat16)


def draw_key_shift(key, part):
    random_children = jax.random.split(key, 6)
    slow_share = 0.5
    slow_heads = jax.random.uniform(random_children[0], (HEADS,), jnp.float32) < slow_share
    slow_level = jax.random.uniform(random_children[1], (HEADS,), jnp.float32, -8.0, -7.0)
    fast_level = jax.random.uniform(random_children[2], (HEADS,), jnp.float32, -4.0, -3.0)
    ground_level = jnp.where(slow_heads, slow_level, fast_level)
    shard_level = jax.random.uniform(random_children[3], (PACKED_TOKENS // SHARD, 1, 1), jnp.float32, -0.8, 0.8)
    portion_rows = jnp.broadcast_to(shard_level, (PACKED_TOKENS // SHARD, SHARD, 1)).reshape(PACKED_TOKENS, 1)
    spike_places = jax.random.randint(random_children[4], (8,), 0, PACKED_TOKENS)
    spike_mask = jnp.any(jnp.arange(PACKED_TOKENS)[:, None] == spike_places[None, :], axis=1)
    spike_rows = jnp.where(spike_mask, 6.5, 0.0)[:, None]
    coarse_estimate = 0.3 * jnp.clip(jax.random.normal(random_children[5], (PACKED_TOKENS, HEADS), jnp.float32), -3.0, 3.0)
    merged_output = ground_level[None, :] + portion_rows + spike_rows + coarse_estimate
    return jnp.clip(merged_output, -10.0, 6.0).astype(jnp.bfloat16)


def draw_stream(key, part):
    base_key, col_key = jax.random.split(key, 2)
    col_scale = jnp.exp(jnp.linspace(-0.916, 0.693, D)) * jax.random.uniform(col_key, (D,), jnp.float32, 0.7, 1.3)
    base_part = jax.random.normal(base_key, (PACKED_TOKENS, D), jnp.float32)
    return jnp.clip(base_part * col_scale[None, :], -8.0, 8.0).astype(jnp.bfloat16)


def block_scale(key, extent, cuts, low, high):
    def one(dim, shards_of):
        heights = jax.random.uniform(jax.random.fold_in(jax.random.fold_in(key, 6), dim), (shards_of,), jnp.float32, low / len(cuts), high / len(cuts))
        return jnp.repeat(jnp.exp(heights), extent[dim] // shards_of).reshape((-1,) + (1,) * (len(extent) - dim - 1))

    factor_of = one(*cuts[0])
    for cut in cuts[1:]:
        factor_of = factor_of * one(*cut)
    return factor_of


def length_profile(amount, total, reach, skew):
    portions = [(1 << 20) // math.isqrt(rank ** skew) + 1 for rank in range(2, amount + 1)]
    surplus, counts = total - reach - (amount - 1), [1] * (amount - 1)
    while surplus > 0:
        movable = [i for i in range(amount - 1) if counts[i] < reach]
        pool, left = sum([portions[i] for i in movable]), surplus
        for i in movable:
            extra = min(reach - counts[i], max(1, left * portions[i] // pool), surplus)
            counts[i] = counts[i] + extra
            surplus = surplus - extra
    return np.array([reach] + counts)


def ragged_sizes(own_key, count, total, limit, lean):
    if count == 2:
        one = jax.random.randint(own_key, (), max(1, total - limit), min(limit, total - 1) + 1)
        return jnp.stack([one, total - one])
    sizes = jnp.asarray(length_profile(count, total, limit, lean), jnp.int32)
    twos = (count - 1) // 2
    giver, receiver = sizes[1:1 + 2 * twos:2], sizes[2:2 + 2 * twos:2]
    room = jnp.minimum(giver - 1, limit - receiver)
    passed = jax.random.randint(jax.random.fold_in(own_key, 1), (twos,), 0, 1 << 20) % (room + 1)
    sizes = sizes.at[1:1 + 2 * twos:2].set(giver - passed).at[2:2 + 2 * twos:2].set(receiver + passed)
    return sizes[jax.random.permutation(jax.random.fold_in(own_key, 2), count)]


def shared_out(rng, own, number, rows, number_of, top, most, lean):
    sequence = jax.random.permutation(rng, number_of)
    packed, ordinary = portions_of(number_of, rows * top, most, lean, True), portions_of(number_of, rows * top, most, lean, False)
    places = jnp.arange(number_of)

    def named(tallies, rotation):
        used = int((tallies > 0).sum())
        fixed = max(1, used // 4)
        moved = fixed + (places - fixed + rotation * (used - fixed)) % max(1, number_of - fixed)
        return jnp.zeros((number_of,), jnp.int32).at[sequence[jnp.where(places < fixed, places, moved)]].set(jnp.asarray(tallies, jnp.int32))

    tallies = jnp.where(number % 4 == 0, named(packed, number // 4), named(ordinary, number - number // 4 - 1))
    mixed = jax.random.permutation(jax.random.fold_in(own, 3), number_of)
    giver, sink = mixed[0:number_of // 2 * 2:2], mixed[1:number_of // 2 * 2:2]
    slack = jnp.minimum(tallies[giver] - 1, most - tallies[sink]) // 2
    slack = jnp.where((giver == sequence[0]) | (sink == sequence[0]) | (tallies[sink] == 0), 0, jnp.maximum(slack, 0))
    moved = jax.random.randint(jax.random.fold_in(own, 4), (number_of // 2,), 0, 1 << 20) % (slack + 1)
    tallies = tallies.at[giver].add(-moved).at[sink].add(moved)
    labels = jnp.searchsorted(jnp.cumsum(tallies), jnp.arange(rows * top), side="right").astype(jnp.int32)
    listing = labels.reshape(top, rows).T
    listing = listing[jax.random.permutation(jax.random.fold_in(own, 1), rows)]
    rotation = jax.random.randint(jax.random.fold_in(own, 2), (rows, 1), 0, top)
    return jnp.take_along_axis(listing, (jnp.arange(top)[None, :] + rotation) % top, axis=1)


def portions_of(amount, total, limit, skew, full):
    loads = [(1 << 20) // math.isqrt(standing ** skew) + 1 for standing in range(1, amount + 1)]
    largest = limit if full else min(limit, max(-(-total // amount), total * loads[0] // sum(loads)))
    least = 1 if total - largest >= amount - 1 else 0
    holding, surplus = [largest] + [least] * (amount - 1), total - largest - least * (amount - 1)
    while surplus > 0:
        free = [i for i in range(1, amount) if holding[i] < largest] or [i for i in range(1, amount) if holding[i] < limit]
        mass, budget = sum([loads[i] for i in free]), surplus
        for i in free:
            addition = min(limit - holding[i], max(1, budget * loads[i] // mass), surplus)
            holding[i] = holding[i] + addition
            surplus = surplus - addition
    return np.array(holding)


def gaussian(key, extent, width, limit, cuts=(), kind=jnp.bfloat16):
    drawn = width * jax.random.normal(key, extent, jnp.float32)
    if cuts:
        drawn = drawn * block_scale(key, extent, cuts, -0.22, 0.18)
    return jnp.clip(drawn, -limit, limit).astype(kind)


def setup_inputs(seed: int = 0) -> dict:
    seeds = jax.random.split(jax.random.key(seed), 14)
    query_rows = gaussian(seeds[0], (PACKED_TOKENS, HEADS * HEAD), 1.0, 6.0, ((0, 8), (1, 4)))
    key_rows = gaussian(seeds[1], (PACKED_TOKENS, HEADS * HEAD), 1.0, 6.0, ((0, 8), (1, 4)))
    value_rows = draw_value_rows(jax.random.fold_in(seeds[13], 71), 0)
    key_shift = draw_key_shift(jax.random.fold_in(seeds[13], 71), 0)
    documents = jnp.searchsorted(jnp.cumsum(ragged_sizes(seeds[4], DOCS, PACKED_TOKENS, DOC_MOST, 2)), jnp.arange(PACKED_TOKENS), side="right").astype(jnp.int32)
    out_weight = gaussian(seeds[5], (HEADS * HEAD, D), (HEADS * HEAD) ** -0.5, 0.1875, ((0, 4),))
    stream = draw_stream(jax.random.fold_in(seeds[13], 71), 0)
    norm_gain = jnp.clip(1.0 + 0.18 * jax.random.normal(seeds[7], (D,), jnp.float32), 0.1, 1.9)
    expert_ids_keys = jax.random.split(jax.random.fold_in(seeds[8], 1), PACKED_TOKENS // SHARD)
    expert_ids_turns = jax.random.permutation(jax.random.fold_in(seeds[8], 3), PACKED_TOKENS // SHARD)
    expert_ids = jax.vmap(lambda own, number: shared_out(jax.random.fold_in(seeds[8], 2), own, number, SHARD, EXPERTS, TOP_K, CAP, 2))(expert_ids_keys, expert_ids_turns).reshape((PACKED_TOKENS, TOP_K))
    expert_weights = jnp.clip(0.25 + 0.75 * jax.random.uniform(seeds[9], (PACKED_TOKENS, TOP_K), jnp.float32) ** block_scale(seeds[9], (PACKED_TOKENS, TOP_K), ((0, 8),), -0.2, 0.2), 0.25, 1.0)
    gate_weight = gaussian(seeds[10], (EXPERTS, D, FF), D ** -0.5, 0.125, ((0, 8), (2, 4)))
    up_weight = gaussian(seeds[11], (EXPERTS, D, FF), D ** -0.5, 0.125, ((0, 8), (2, 4)))
    down_weight = gaussian(seeds[12], (EXPERTS, FF, D), FF ** -0.5, 0.09375, ((0, 8), (1, 4)))
    return {"query_rows": query_rows, "key_rows": key_rows, "value_rows": value_rows, "key_shift": key_shift, "documents": documents, "out_weight": out_weight, "stream": stream, "norm_gain": norm_gain, "expert_ids": expert_ids, "expert_weights": expert_weights, "gate_weight": gate_weight, "up_weight": up_weight, "down_weight": down_weight}


NORM_EPS = 1e-06

def reference(query_rows, key_rows, value_rows, key_shift, documents, out_weight, stream, norm_gain, expert_ids, expert_weights, gate_weight, up_weight, down_weight):
    front_pad = REACH * SHARD
    window = front_pad + SHARD
    query_heads = query_rows.astype(jnp.float32).reshape(PACKED_TOKENS, HEADS, HEAD)
    key_heads = jnp.pad(key_rows.astype(jnp.float32).reshape(PACKED_TOKENS, HEADS, HEAD), ((front_pad, 0), (0, 0), (0, 0)))
    value_heads = jnp.pad(value_rows.astype(jnp.float32).reshape(PACKED_TOKENS, HEADS, HEAD), ((front_pad, 0), (0, 0), (0, 0)))
    shift_pad = jnp.pad(key_shift.astype(jnp.float32), ((front_pad, 0), (0, 0)))
    doc_pad = jnp.pad(documents, (front_pad, 0), constant_values=-1)

    def attend_block(block_index):
        begin_row = (block_index * SHARD).astype(jnp.int32)
        query_block = lax.dynamic_slice_in_dim(query_heads, begin_row, SHARD, 0)
        query_docs = lax.dynamic_slice_in_dim(documents, begin_row, SHARD, 0)
        key_window = lax.dynamic_slice_in_dim(key_heads, begin_row, window, 0)
        value_window = lax.dynamic_slice_in_dim(value_heads, begin_row, window, 0)
        shift_window = lax.dynamic_slice_in_dim(shift_pad, begin_row, window, 0)
        key_docs = lax.dynamic_slice_in_dim(doc_pad, begin_row, window, 0)
        query_pos = begin_row + jnp.arange(SHARD, dtype=jnp.int32)
        key_pos = begin_row - front_pad + jnp.arange(window, dtype=jnp.int32)
        scores = jnp.einsum('qhd,khd->hqk', query_block, key_window) * HEAD ** (-0.5)
        scores = scores + jnp.transpose(shift_window)[:, None, :]
        admitted = (key_pos[None, :] < query_pos[:, None]) & (key_docs[None, :] == query_docs[:, None])
        log_rest = jnp.where(admitted[None], jax.nn.log_sigmoid(-scores), 0.0)
        log_after = lax.cumsum(log_rest, axis=2, reverse=True) - log_rest
        stick_weight = jnp.where(admitted[None], jnp.exp(jax.nn.log_sigmoid(scores) + log_after), 0.0).astype(jnp.bfloat16)
        stick_weight = lax.optimization_barrier(stick_weight).astype(jnp.float32)
        attended = jnp.einsum('hqk,khd->qhd', stick_weight, value_window)
        return attended.reshape(SHARD, HEADS * HEAD).astype(jnp.bfloat16)
    attended = lax.map(attend_block, jnp.arange(N_SP, dtype=jnp.int32)).reshape(PACKED_TOKENS, HEADS * HEAD)
    group_width = HEADS * HEAD // N_TP
    projected = jnp.zeros((PACKED_TOKENS, D), jnp.float32)
    for part_index in range(N_TP):
        lower = part_index * group_width
        partial_value = jnp.dot(attended[:, lower:lower + group_width], out_weight[lower:lower + group_width], preferred_element_type=jnp.float32)
        projected = projected + lax.optimization_barrier(partial_value.astype(jnp.bfloat16)).astype(jnp.float32)
    middle = (stream.astype(jnp.float32) + projected).astype(jnp.bfloat16)
    middle_wide = lax.optimization_barrier(middle).astype(jnp.float32)
    inv_rms = lax.rsqrt(lax.optimization_barrier(jnp.mean(middle_wide * middle_wide, axis=1, keepdims=True)) + NORM_EPS)
    normed = (middle_wide * inv_rms * norm_gain[None, :]).astype(jnp.bfloat16)
    flat_ids = expert_ids.reshape(N_SP, SHARD * TOP_K).astype(jnp.int32)
    onehot = (flat_ids[:, :, None] == jnp.arange(EXPERTS, dtype=jnp.int32)[None, None, :]).astype(jnp.int32)
    slot_index = lax.optimization_barrier(jnp.sum((jnp.cumsum(onehot, axis=1) - 1) * onehot, axis=2)).astype(jnp.int32)
    source = jnp.broadcast_to(jnp.arange(N_SP, dtype=jnp.int32)[:, None], flat_ids.shape)
    token_index = source * SHARD + jnp.arange(SHARD * TOP_K, dtype=jnp.int32)[None, :] // TOP_K
    table = jnp.zeros((EXPERTS, N_SP, CAP), jnp.int32).at[flat_ids, source, slot_index].set(token_index)
    filled = jnp.zeros((EXPERTS, N_SP, CAP), jnp.int32).at[flat_ids, source, slot_index].set(1)
    hidden_group = FF // N_TP

    def run_expert(expert_index):
        row_index = table[expert_index].reshape(N_SP * CAP)
        used = filled[expert_index].reshape(N_SP * CAP, 1) > 0
        row_block = jnp.where(used, normed[row_index], jnp.zeros((), jnp.bfloat16))
        gate_value = jnp.dot(row_block, gate_weight[expert_index], preferred_element_type=jnp.float32)
        up_value = jnp.dot(row_block, up_weight[expert_index], preferred_element_type=jnp.float32)
        hidden = (jax.nn.silu(gate_value) * up_value).astype(jnp.bfloat16)
        summed = jnp.zeros((N_SP * CAP, D), jnp.float32)
        for part_index in range(N_TP):
            lower = part_index * hidden_group
            partial_value = jnp.dot(hidden[:, lower:lower + hidden_group], down_weight[expert_index, lower:lower + hidden_group], preferred_element_type=jnp.float32)
            summed = summed + lax.optimization_barrier(partial_value.astype(jnp.bfloat16)).astype(jnp.float32)
        return summed.astype(jnp.bfloat16)
    expert_out = lax.map(run_expert, jnp.arange(EXPERTS, dtype=jnp.int32))
    flat_pos = (flat_ids * (N_SP * CAP) + source * CAP + slot_index).reshape(PACKED_TOKENS * TOP_K)
    picked = expert_out.reshape(EXPERTS * N_SP * CAP, D)[flat_pos].astype(jnp.float32).reshape(PACKED_TOKENS, TOP_K, D)
    mixed = lax.optimization_barrier(jnp.sum(picked * expert_weights[:, :, None], axis=1))
    return (middle_wide + mixed).astype(jnp.bfloat16)
```

```python
import functools

import jax
import jax.numpy as jnp
from jax import lax
from jax.experimental import pallas as pl
from jax.experimental.pallas import tpu as pltpu
from jax.sharding import PartitionSpec as P

D = 2048
HEAD = 64
REACH = 4
LANES = 128
LOG2E = 1.4426950408889634

NORM_EPS = 1e-06
MESH = pl.DeviceIdType.MESH


def attention_kernel(
    count, q_ref, qdoc_ref, kv_ref, aux_ref, out_ref,
    kv_buf, aux_buf, acc, total, kv_send, kv_recv, aux_send, aux_recv,
):
    me = lax.axis_index("sp")
    odd = lax.rem(me, 2)
    even = 1 - odd
    partner = me + 1 - 2 * odd
    pairs, rows, _ = kv_ref.shape

    barrier = pltpu.get_barrier_semaphore()
    pl.semaphore_signal(barrier, inc=1, device_id={"sp": partner}, device_id_type=MESH)

    @pl.when(me + 2 < count)
    def _():
        pl.semaphore_signal(barrier, inc=1, device_id={"sp": me + 2}, device_id_type=MESH)

    @pl.when(me >= 2)
    def _():
        pl.semaphore_signal(barrier, inc=1, device_id={"sp": me - 2}, device_id_type=MESH)

    peers = 1 + jnp.where(me + 2 < count, 1, 0) + jnp.where(me >= 2, 1, 0)
    pl.semaphore_wait(barrier, peers)

    def own(item):
        return kv_ref.at[item] if item < pairs else aux_ref

    def slot(item, distance):
        return kv_buf.at[distance - 1, item] if item < pairs else aux_buf.at[distance - 1]

    def remote(item, source, distance, kind, target):
        if item < pairs:
            send, recv = kv_send.at[kind, item], kv_recv.at[distance - 1, item]
        else:
            send, recv = aux_send.at[kind], aux_recv.at[distance - 1]
        return pltpu.make_async_remote_copy(
            src_ref=source, dst_ref=slot(item, distance), send_sem=send, recv_sem=recv,
            device_id={"sp": target}, device_id_type=MESH,
        )

    has_next = me + 2 < count
    copies = {
        "chain": (has_next, lambda i: remote(i, own(i), 2, 0, me + 2)),
        "chain2": (has_next & (me >= 2), lambda i: remote(i, slot(i, 2), 4, 1, me + 2)),
        "even1": (even == 1, lambda i: remote(i, own(i), 1, 2, partner)),
        "even3": ((even == 1) & (me >= 2), lambda i: remote(i, slot(i, 2), 3, 3, partner)),
        "odd1": ((odd == 1) & (me >= 2), lambda i: remote(i, slot(i, 2), 1, 2, partner)),
        "odd3": ((odd == 1) & (me >= 4), lambda i: remote(i, slot(i, 4), 3, 3, partner)),
    }

    def start(name, items):
        condition, make = copies[name]

        @pl.when(condition)
        def _():
            for item in items:
                make(item).start()

    def arrive(distance, items):
        @pl.when(me >= distance)
        def _():
            for item in items:
                remote(item, slot(item, distance), distance, 0, partner).wait_recv()

    lane = lax.broadcasted_iota(jnp.int32, (rows, LANES), 1)
    row_of = lax.broadcasted_iota(jnp.int32, (rows, rows), 0)
    col_of = lax.broadcasted_iota(jnp.int32, (rows, rows), 1)
    later = jnp.where(row_of >= col_of, 1.0, 0.0).astype(jnp.bfloat16)
    qdoc = qdoc_ref[...]
    per_pair = LANES // HEAD

    def block(head, pair, half, distance, key_value, aux, aux_row):
        in_head = (lane >= half * HEAD) & (lane < (half + 1) * HEAD)
        cols = pl.ds(pair * LANES, LANES)
        query = q_ref[:, cols]
        query = jnp.where(in_head, query, jnp.zeros_like(query))
        scores = lax.dot_general(
            query, key_value[:, :LANES], (((1,), (1,)), ((), ())),
            preferred_element_type=jnp.float32,
        )
        scores = (scores * (HEAD ** -0.5) + aux_row(head)) * LOG2E
        admitted = qdoc == aux_row(aux.shape[0] - 1)
        if distance == 0:
            admitted = admitted & (col_of < row_of)
        rest = jnp.minimum(-scores, 0.0) - jnp.log2(1.0 + jnp.exp2(-jnp.abs(scores)))
        rest = jnp.where(admitted, rest, 0.0)
        high = rest.astype(jnp.bfloat16)
        low = (rest - high.astype(jnp.float32)).astype(jnp.bfloat16)
        suffix = jnp.dot(high, later, preferred_element_type=jnp.float32) + jnp.dot(
            low, later, preferred_element_type=jnp.float32
        )
        before = jnp.zeros((rows, 1), jnp.float32) if distance == 0 else total[head]
        weight = jnp.where(admitted, jnp.exp2(scores + suffix + before), 0.0).astype(jnp.bfloat16)
        product = jnp.dot(weight, key_value[:, LANES:], preferred_element_type=jnp.float32)
        product = jnp.where(in_head, product, 0.0)
        if distance == 0 and half == 0:
            acc[pair] = product
        else:
            acc[pair] += product
        total[head] = before + suffix[:, :1]

    def own_pair(pair):
        for half in range(per_pair):
            block(
                pair * per_pair + half, pair, half, 0, kv_ref[pair], aux_ref,
                lambda r: aux_ref[pl.ds(r, 1), :],
            )

    def far_pair(pair, distance):
        @pl.when(me >= distance)
        def _():
            for half in range(per_pair):
                block(
                    pair * per_pair + half, pair, half, distance,
                    kv_buf[distance - 1, pair], aux_buf.at[distance - 1],
                    lambda r: aux_buf[distance - 1, pl.ds(r, 1), :],
                )

    everything = (pairs,) + tuple(range(pairs))
    start("chain", everything)
    start("even1", everything)
    first, rest_items = (pairs, 0), tuple(range(1, pairs))
    own_pair(0)
    arrive(2, first)
    for name in ("chain2", "even3", "odd1"):
        start(name, first)
    for pair in range(1, pairs):
        own_pair(pair)
    arrive(2, rest_items)
    for name in ("chain2", "even3", "odd1"):
        start(name, rest_items)
    arrive(1, first)
    far_pair(0, 1)
    far_pair(0, 2)
    arrive(4, first)
    start("odd3", first)
    arrive(1, rest_items)
    for pair in range(1, pairs):
        far_pair(pair, 1)
        far_pair(pair, 2)
    arrive(4, rest_items)
    start("odd3", rest_items)
    arrive(3, first)
    far_pair(0, 3)
    far_pair(0, 4)
    arrive(3, rest_items)
    for pair in range(1, pairs):
        far_pair(pair, 3)
        far_pair(pair, 4)
    for pair in range(pairs):
        out_ref[:, pair * LANES:(pair + 1) * LANES] = acc[pair].astype(out_ref.dtype)
    for condition, make in copies.values():
        @pl.when(condition)
        def _(make=make):
            for item in everything:
                make(item).wait_send()


def attend(query_rows, key_rows, value_rows, key_shift, documents):
    count = lax.axis_size("sp")
    rows, width = query_rows.shape
    pairs = width // LANES
    key_value = jnp.stack([
        jnp.concatenate(
            [part[:, p * LANES:(p + 1) * LANES] for part in (key_rows, value_rows)], axis=1
        )
        for p in range(pairs)
    ])
    heads = key_shift.shape[1]
    docs = documents.astype(jnp.float32)
    aux = jnp.concatenate([
        jnp.transpose(key_shift).astype(jnp.float32),
        jnp.broadcast_to(docs[None, :], (8 - heads % 8, rows)),
    ])
    vmem = pl.BlockSpec(memory_space=pltpu.VMEM)
    return pl.pallas_call(
        functools.partial(attention_kernel, count),
        out_shape=jax.ShapeDtypeStruct((rows, width), jnp.bfloat16),
        in_specs=[vmem] * 4,
        out_specs=vmem,
        scratch_shapes=[
            pltpu.VMEM((REACH, pairs, rows, 2 * LANES), jnp.bfloat16),
            pltpu.VMEM((REACH,) + aux.shape, jnp.float32),
            pltpu.VMEM((pairs, rows, LANES), jnp.float32),
            pltpu.VMEM((heads, rows, 1), jnp.float32),
            pltpu.SemaphoreType.DMA((4, pairs)),
            pltpu.SemaphoreType.DMA((REACH, pairs)),
            pltpu.SemaphoreType.DMA((4,)),
            pltpu.SemaphoreType.DMA((REACH,)),
        ],
        compiler_params=pltpu.CompilerParams(collective_id=0, has_side_effects=True),
        name="attention",
    )(query_rows, docs[:, None], key_value, aux)


def shards(
    query_rows,
    key_rows,
    value_rows,
    key_shift,
    documents,
    out_weight,
    stream,
    norm_gain,
    expert_ids,
    expert_weights,
    gate_weight,
    up_weight,
    down_weight,
):
    portion_rows = query_rows.shape[0]
    attended = attend(query_rows, key_rows, value_rows, key_shift, documents)
    partial_value = jnp.dot(attended, out_weight, preferred_element_type=jnp.float32)
    projected = lax.psum_scatter(
        partial_value.astype(jnp.bfloat16), "tp", scatter_dimension=1, tiled=True
    ).astype(jnp.float32)
    middle = (stream.astype(jnp.float32) + projected).astype(jnp.bfloat16)
    middle_wide = middle.astype(jnp.float32)
    sending = middle
    top_count = expert_ids.shape[1]
    experts = lax.axis_size("sp") * gate_weight.shape[0]
    capacity = (4 * portion_rows * top_count + 3 * experts - 1) // (3 * experts)
    flat_ids = expert_ids.reshape(portion_rows * top_count)
    onehot = (flat_ids[:, None] == jnp.arange(experts, dtype=jnp.int32)[None, :]).astype(jnp.int32)
    slot_index = jnp.sum((jnp.cumsum(onehot, axis=0) - 1) * onehot, axis=1)
    target = flat_ids * capacity + slot_index
    buffer = jnp.zeros((experts * capacity, sending.shape[1]), jnp.bfloat16)
    buffer = buffer.at[target].set(jnp.repeat(sending, top_count, axis=0))
    buffer = buffer.reshape(experts, capacity, sending.shape[1])
    arrived = lax.all_to_all(buffer, "sp", split_axis=0, concat_axis=0, tiled=True)
    arrived = lax.all_gather(arrived, "tp", axis=2, tiled=True)
    sources, item_count, feat_count = arrived.shape
    row_block = arrived.reshape(sources * item_count, feat_count).astype(jnp.float32)
    square_mean = jnp.sum(row_block * row_block, axis=1, keepdims=True) / D
    row_block = (row_block * lax.rsqrt(square_mean + NORM_EPS) * norm_gain[None, :]).astype(
        jnp.bfloat16
    )
    gate_value = jnp.dot(row_block, gate_weight[0], preferred_element_type=jnp.float32)
    up_value = jnp.dot(row_block, up_weight[0], preferred_element_type=jnp.float32)
    hidden = (jax.nn.silu(gate_value) * up_value).astype(jnp.bfloat16)
    partial_out = jnp.dot(hidden, down_weight[0], preferred_element_type=jnp.float32)
    summed = lax.psum_scatter(
        partial_out.astype(jnp.bfloat16), "tp", scatter_dimension=1, tiled=True
    ).astype(jnp.float32)
    result = summed.astype(jnp.bfloat16).reshape(sources, item_count, summed.shape[1])
    returned_rows = lax.all_to_all(result, "sp", split_axis=0, concat_axis=0, tiled=True)
    picked = returned_rows.reshape(experts * capacity, returned_rows.shape[2])[target].astype(
        jnp.float32
    )
    mixed = jnp.sum(
        picked.reshape(portion_rows, top_count, picked.shape[1]) * expert_weights[:, :, None],
        axis=1,
    )
    return (middle_wide + mixed).astype(jnp.bfloat16)


def solution(mesh):
    in_specs = (
        P("sp", "tp"),
        P("sp", "tp"),
        P("sp", "tp"),
        P("sp", "tp"),
        P("sp"),
        P("tp", None),
        P("sp", "tp"),
        P(),
        P("sp", None),
        P("sp", None),
        P("sp", None, "tp"),
        P("sp", None, "tp"),
        P("sp", "tp", None),
    )
    out_specs = P("sp", "tp")
    return jax.shard_map(shards, mesh=mesh, in_specs=in_specs, out_specs=out_specs, check_vma=False)
```

```python
import functools

import jax
import jax.numpy as jnp
from jax import lax
from jax.experimental import pallas as pl
from jax.experimental.pallas import tpu as pltpu
from jax.sharding import PartitionSpec as P

HEAD = 64
REACH = 4
LANES = 128
LOG2E = 1.4426950408889634

NORM_EPS = 1e-06
MESH = pl.DeviceIdType.MESH


def attention_kernel(
    count, q_ref, qdoc_ref, kv_ref, aux_ref, out_ref,
    kv_buf, aux_buf, acc, total, kv_send, kv_recv, aux_send, aux_recv,
):
    me = lax.axis_index("sp")
    odd = lax.rem(me, 2)
    even = 1 - odd
    partner = me + 1 - 2 * odd
    pairs, rows, _ = kv_ref.shape

    barrier = pltpu.get_barrier_semaphore()
    pl.semaphore_signal(barrier, inc=1, device_id={"sp": partner}, device_id_type=MESH)

    @pl.when(me + 2 < count)
    def _():
        pl.semaphore_signal(barrier, inc=1, device_id={"sp": me + 2}, device_id_type=MESH)

    @pl.when(me >= 2)
    def _():
        pl.semaphore_signal(barrier, inc=1, device_id={"sp": me - 2}, device_id_type=MESH)

    peers = 1 + jnp.where(me + 2 < count, 1, 0) + jnp.where(me >= 2, 1, 0)
    pl.semaphore_wait(barrier, peers)

    def own(item):
        return kv_ref.at[item] if item < pairs else aux_ref

    def slot(item, distance):
        return kv_buf.at[distance - 1, item] if item < pairs else aux_buf.at[distance - 1]

    def remote(item, source, distance, kind, target):
        if item < pairs:
            send, recv = kv_send.at[kind, item], kv_recv.at[distance - 1, item]
        else:
            send, recv = aux_send.at[kind], aux_recv.at[distance - 1]
        return pltpu.make_async_remote_copy(
            src_ref=source, dst_ref=slot(item, distance), send_sem=send, recv_sem=recv,
            device_id={"sp": target}, device_id_type=MESH,
        )

    has_next = me + 2 < count
    copies = {
        "chain": (has_next, lambda i: remote(i, own(i), 2, 0, me + 2)),
        "chain2": (has_next & (me >= 2), lambda i: remote(i, slot(i, 2), 4, 1, me + 2)),
        "even1": (even == 1, lambda i: remote(i, own(i), 1, 2, partner)),
        "even3": ((even == 1) & (me >= 2), lambda i: remote(i, slot(i, 2), 3, 3, partner)),
        "odd1": ((odd == 1) & (me >= 2), lambda i: remote(i, slot(i, 2), 1, 2, partner)),
        "odd3": ((odd == 1) & (me >= 4), lambda i: remote(i, slot(i, 4), 3, 3, partner)),
    }

    def start(name, items):
        condition, make = copies[name]

        @pl.when(condition)
        def _():
            for item in items:
                make(item).start()

    def arrive(distance, items):
        @pl.when(me >= distance)
        def _():
            for item in items:
                remote(item, slot(item, distance), distance, 0, partner).wait_recv()

    lane = lax.broadcasted_iota(jnp.int32, (rows, LANES), 1)
    row_of = lax.broadcasted_iota(jnp.int32, (rows, rows), 0)
    col_of = lax.broadcasted_iota(jnp.int32, (rows, rows), 1)
    later = jnp.where(row_of >= col_of, 1.0, 0.0).astype(jnp.bfloat16)
    qdoc = qdoc_ref[...]
    per_pair = LANES // HEAD

    def block(head, pair, half, distance, key_value, aux, aux_row):
        in_head = (lane >= half * HEAD) & (lane < (half + 1) * HEAD)
        cols = pl.ds(pair * LANES, LANES)
        query = q_ref[:, cols]
        query = jnp.where(in_head, query, jnp.zeros_like(query))
        scores = lax.dot_general(
            query, key_value[:, :LANES], (((1,), (1,)), ((), ())),
            preferred_element_type=jnp.float32,
        )
        scores = (scores * (HEAD ** -0.5) + aux_row(head)) * LOG2E
        admitted = qdoc == aux_row(aux.shape[0] - 1)
        if distance == 0:
            admitted = admitted & (col_of < row_of)
        rest = jnp.minimum(-scores, 0.0) - jnp.log2(1.0 + jnp.exp2(-jnp.abs(scores)))
        rest = jnp.where(admitted, rest, 0.0)
        high = rest.astype(jnp.bfloat16)
        low = (rest - high.astype(jnp.float32)).astype(jnp.bfloat16)
        suffix = jnp.dot(high, later, preferred_element_type=jnp.float32) + jnp.dot(
            low, later, preferred_element_type=jnp.float32
        )
        before = jnp.zeros((rows, 1), jnp.float32) if distance == 0 else total[head]
        weight = jnp.where(admitted, jnp.exp2(scores + suffix + before), 0.0).astype(jnp.bfloat16)
        product = jnp.dot(weight, key_value[:, LANES:], preferred_element_type=jnp.float32)
        product = jnp.where(in_head, product, 0.0)
        if distance == 0 and half == 0:
            acc[pair] = product
        else:
            acc[pair] += product
        total[head] = before + suffix[:, :1]

    def own_pair(pair):
        for half in range(per_pair):
            block(
                pair * per_pair + half, pair, half, 0, kv_ref[pair], aux_ref,
                lambda r: aux_ref[pl.ds(r, 1), :],
            )

    def far_pair(pair, distance):
        @pl.when(me >= distance)
        def _():
            for half in range(per_pair):
                block(
                    pair * per_pair + half, pair, half, distance,
                    kv_buf[distance - 1, pair], aux_buf.at[distance - 1],
                    lambda r: aux_buf[distance - 1, pl.ds(r, 1), :],
                )

    everything = (pairs,) + tuple(range(pairs))
    start("chain", everything)
    start("even1", everything)
    first, rest_items = (pairs, 0), tuple(range(1, pairs))
    own_pair(0)
    arrive(2, first)
    for name in ("chain2", "even3", "odd1"):
        start(name, first)
    for pair in range(1, pairs):
        own_pair(pair)
    arrive(2, rest_items)
    for name in ("chain2", "even3", "odd1"):
        start(name, rest_items)
    arrive(1, first)
    far_pair(0, 1)
    far_pair(0, 2)
    arrive(4, first)
    start("odd3", first)
    arrive(1, rest_items)
    for pair in range(1, pairs):
        far_pair(pair, 1)
        far_pair(pair, 2)
    arrive(4, rest_items)
    start("odd3", rest_items)
    arrive(3, first)
    far_pair(0, 3)
    far_pair(0, 4)
    arrive(3, rest_items)
    for pair in range(1, pairs):
        far_pair(pair, 3)
        far_pair(pair, 4)
    for pair in range(pairs):
        out_ref[:, pair * LANES:(pair + 1) * LANES] = acc[pair].astype(out_ref.dtype)
    for condition, make in copies.values():
        @pl.when(condition)
        def _(make=make):
            for item in everything:
                make(item).wait_send()


def attend(query_rows, key_rows, value_rows, key_shift, documents):
    count = lax.axis_size("sp")
    rows, width = query_rows.shape
    pairs = width // LANES
    key_value = jnp.stack([
        jnp.concatenate(
            [part[:, p * LANES:(p + 1) * LANES] for part in (key_rows, value_rows)], axis=1
        )
        for p in range(pairs)
    ])
    heads = key_shift.shape[1]
    docs = documents.astype(jnp.float32)
    aux = jnp.concatenate([
        jnp.transpose(key_shift).astype(jnp.float32),
        jnp.broadcast_to(docs[None, :], (8 - heads % 8, rows)),
    ])
    vmem = pl.BlockSpec(memory_space=pltpu.VMEM)
    return pl.pallas_call(
        functools.partial(attention_kernel, count),
        out_shape=jax.ShapeDtypeStruct((rows, width), jnp.bfloat16),
        in_specs=[vmem] * 4,
        out_specs=vmem,
        scratch_shapes=[
            pltpu.VMEM((REACH, pairs, rows, 2 * LANES), jnp.bfloat16),
            pltpu.VMEM((REACH,) + aux.shape, jnp.float32),
            pltpu.VMEM((pairs, rows, LANES), jnp.float32),
            pltpu.VMEM((heads, rows, 1), jnp.float32),
            pltpu.SemaphoreType.DMA((4, pairs)),
            pltpu.SemaphoreType.DMA((REACH, pairs)),
            pltpu.SemaphoreType.DMA((4,)),
            pltpu.SemaphoreType.DMA((REACH,)),
        ],
        compiler_params=pltpu.CompilerParams(collective_id=0, has_side_effects=True),
        name="attention",
    )(query_rows, docs[:, None], key_value, aux)


def greet(count, others):
    me = lax.axis_index("sp")
    barrier = pltpu.get_barrier_semaphore()

    def signal(r, carry):
        pl.semaphore_signal(
            barrier, inc=1, device_id={"sp": lax.rem(me + r, count)}, device_id_type=MESH
        )
        return carry

    if count > 1:
        lax.fori_loop(1, count, signal, 0)
    for other in others:
        pl.semaphore_signal(barrier, inc=1, device_id={"tp": other}, device_id_type=MESH)
    pl.semaphore_wait(barrier, count - 1 + len(others))


def each(low, high, body):
    def step(r, carry):
        body(r)
        return carry

    lax.fori_loop(low, high, step, 0)


def neighbours():
    t = lax.axis_index("tp")
    return t, t + 1 - 2 * lax.rem(t, 2), lax.rem(t + 2, lax.axis_size("tp"))


def dispatch_kernel(count, in_ref, gain_ref, out_ref, held, send, recv):
    me = lax.axis_index("sp")
    t, partner, across = neighbours()
    _, capacity, feats = in_ref.shape
    features = held.shape[2]
    greet(count, (partner, across))

    def columns(owner):
        return pl.ds(pl.multiple_of(owner * feats, feats), feats)

    def source(r):
        return lax.rem(me - r + count, count)

    def arrival(r):
        target = lax.rem(me + r, count)
        return pltpu.make_async_remote_copy(
            src_ref=in_ref.at[target], dst_ref=held.at[me, :, columns(t)],
            send_sem=send.at[0, r], recv_sem=recv.at[0, r],
            device_id={"sp": target}, device_id_type=MESH,
        )

    def share(r, kind, owner, target):
        place = held.at[source(r), :, columns(owner)]
        return pltpu.make_async_remote_copy(
            src_ref=place, dst_ref=place, send_sem=send.at[kind, r], recv_sem=recv.at[kind, r],
            device_id={"tp": target}, device_id_type=MESH,
        )

    def cross(r):
        return share(r, 1, t, across)

    def pair(r):
        return share(r, 2, t, partner)

    def relay(r):
        return share(r, 3, across, partner)

    def spread(r):
        cross(r).start()
        pair(r).start()

    def norm(r):
        pair(r).wait_recv()
        relay(r).wait_recv()
        row_block = held[source(r)].astype(jnp.float32)
        square_mean = jnp.sum(row_block * row_block, axis=1, keepdims=True) / features
        out_ref[source(r)] = (
            row_block * lax.rsqrt(square_mean + NORM_EPS) * gain_ref[...]
        ).astype(out_ref.dtype)

    each(1, count, lambda r: arrival(r).start())
    local = pltpu.make_async_copy(in_ref.at[me], held.at[me, :, columns(t)], send.at[0, 0])
    local.start()
    local.wait()
    spread(0)

    def take(r):
        arrival(r).wait_recv()
        spread(r)

    each(1, count, take)

    def forward(r):
        cross(r).wait_recv()
        relay(r).start()

    forward(0)

    def finish(r):
        forward(r)
        norm(r - 1)

    each(1, count, finish)
    norm(count - 1)
    each(1, count, lambda r: arrival(r).wait_send())

    def drain(r):
        cross(r).wait_send()
        pair(r).wait_send()
        relay(r).wait_send()

    each(0, count, drain)


def reduce_kernel(count, back, in_ref, out_ref, near, outgoing, far, final, send, recv):
    me = lax.axis_index("sp")
    t, partner, across = neighbours()
    partner_across = lax.rem(partner + 2, lax.axis_size("tp"))
    blocks, rows, _ = in_ref.shape
    feats = out_ref.shape[2]
    greet(count if back else 1, (partner, across))

    def columns(owner):
        return pl.ds(pl.multiple_of(owner * feats, feats), feats)

    def place(r):
        return lax.rem(me + r + 1, blocks) if back else r

    def pair(r, which, owner):
        return pltpu.make_async_remote_copy(
            src_ref=in_ref.at[place(r), :, columns(owner)], dst_ref=near.at[which, r],
            send_sem=send.at[which, r], recv_sem=recv.at[which, r],
            device_id={"tp": partner}, device_id_type=MESH,
        )

    def cross(r):
        return pltpu.make_async_remote_copy(
            src_ref=outgoing.at[r], dst_ref=far.at[r],
            send_sem=send.at[2, r], recv_sem=recv.at[2, r],
            device_id={"tp": across}, device_id_type=MESH,
        )

    def home(r):
        return pltpu.make_async_remote_copy(
            src_ref=final.at[r], dst_ref=out_ref.at[me],
            send_sem=send.at[3, r], recv_sem=recv.at[3, r],
            device_id={"sp": place(r)}, device_id_type=MESH,
        )

    def start_pair(r):
        pair(r, 0, partner_across).start()
        pair(r, 1, partner).start()

    each(0, blocks, start_pair)

    def halve(r):
        pair(r, 0, partner_across).wait_recv()
        outgoing[r] = (
            in_ref[place(r), :, columns(across)].astype(jnp.float32)
            + near[0, r].astype(jnp.float32)
        ).astype(outgoing.dtype)
        cross(r).start()

    each(0, blocks, halve)

    def total(r):
        pair(r, 1, partner).wait_recv()
        cross(r).wait_recv()
        return (
            in_ref[place(r), :, columns(t)].astype(jnp.float32)
            + near[1, r].astype(jnp.float32)
            + far[r].astype(jnp.float32)
        ).astype(out_ref.dtype)

    def drain(r):
        pair(r, 0, partner_across).wait_send()
        pair(r, 1, partner).wait_send()
        cross(r).wait_send()

    if back:
        def finish(r):
            final[r] = total(r)
            home(r).start()

        each(0, blocks - 1, finish)
        out_ref[me] = total(blocks - 1)

        def collect(r):
            home(r).wait_recv()
            home(r).wait_send()

        each(0, blocks - 1, collect)
    else:
        def finish(r):
            out_ref[r] = total(r)

        each(0, blocks, finish)
    each(0, blocks, drain)


def dispatch(blocks, norm_gain):
    count, capacity, feats = blocks.shape
    features = norm_gain.shape[0]
    vmem = pl.BlockSpec(memory_space=pltpu.VMEM)
    return pl.pallas_call(
        functools.partial(dispatch_kernel, count),
        out_shape=jax.ShapeDtypeStruct((count, capacity, features), jnp.bfloat16),
        in_specs=[vmem] * 2,
        out_specs=vmem,
        scratch_shapes=[
            pltpu.VMEM((count, capacity, features), jnp.bfloat16),
            pltpu.SemaphoreType.DMA((4, count)),
            pltpu.SemaphoreType.DMA((4, count)),
        ],
        compiler_params=pltpu.CompilerParams(collective_id=1, has_side_effects=True),
        name="dispatch",
    )(blocks, norm_gain[None, :])


def reduce_tp(partial, back, collective_id):
    blocks, rows, features = partial.shape
    feats = features // lax.axis_size("tp")
    vmem = pl.BlockSpec(memory_space=pltpu.VMEM)
    slots = pltpu.VMEM((blocks, rows, feats), jnp.bfloat16)
    return pl.pallas_call(
        functools.partial(reduce_kernel, lax.axis_size("sp"), back),
        out_shape=jax.ShapeDtypeStruct((blocks, rows, feats), jnp.bfloat16),
        in_specs=[vmem],
        out_specs=vmem,
        scratch_shapes=[
            pltpu.VMEM((2, blocks, rows, feats), jnp.bfloat16),
            slots,
            slots,
            slots if back else pltpu.VMEM((8, 128), jnp.bfloat16),
            pltpu.SemaphoreType.DMA((4, blocks)),
            pltpu.SemaphoreType.DMA((4, blocks)),
        ],
        compiler_params=pltpu.CompilerParams(collective_id=collective_id, has_side_effects=True),
        name="combine" if back else "project",
    )(partial)


def shards(
    query_rows,
    key_rows,
    value_rows,
    key_shift,
    documents,
    out_weight,
    stream,
    norm_gain,
    expert_ids,
    expert_weights,
    gate_weight,
    up_weight,
    down_weight,
):
    portion_rows = query_rows.shape[0]
    attended = attend(query_rows, key_rows, value_rows, key_shift, documents)
    partial_value = jnp.dot(attended, out_weight, preferred_element_type=jnp.float32).astype(
        jnp.bfloat16
    )
    cuts = 4 if portion_rows % 64 == 0 else 1
    projected = reduce_tp(
        partial_value.reshape(cuts, portion_rows // cuts, partial_value.shape[1]), False, 2
    ).reshape(portion_rows, stream.shape[1])
    middle = (stream.astype(jnp.float32) + projected.astype(jnp.float32)).astype(jnp.bfloat16)
    top_count = expert_ids.shape[1]
    experts = lax.axis_size("sp") * gate_weight.shape[0]
    capacity = (4 * portion_rows * top_count + 3 * experts - 1) // (3 * experts)
    capacity = (capacity + 15) // 16 * 16
    flat_ids = expert_ids.reshape(portion_rows * top_count)
    onehot = (flat_ids[:, None] == jnp.arange(experts, dtype=jnp.int32)[None, :]).astype(jnp.int32)
    slot_index = jnp.sum((jnp.cumsum(onehot, axis=0) - 1) * onehot, axis=1)
    target = (flat_ids * capacity + slot_index).reshape(portion_rows, top_count)
    slots = jnp.arange(experts * capacity, dtype=jnp.int32)
    placed = target[:, 0][None, :] == slots[:, None]
    for k in range(1, top_count):
        placed = placed | (target[:, k][None, :] == slots[:, None])
    blocks = jnp.dot(
        placed.astype(jnp.bfloat16), middle, preferred_element_type=jnp.float32
    ).astype(jnp.bfloat16)
    arrived = dispatch(blocks.reshape(experts, capacity, middle.shape[1]), norm_gain)
    row_block = arrived.reshape(experts * capacity, arrived.shape[2])
    gate_value = jnp.dot(row_block, gate_weight[0], preferred_element_type=jnp.float32)
    up_value = jnp.dot(row_block, up_weight[0], preferred_element_type=jnp.float32)
    hidden = (jax.nn.silu(gate_value) * up_value).astype(jnp.bfloat16)
    partial_out = jnp.dot(hidden, down_weight[0], preferred_element_type=jnp.float32)
    returned = reduce_tp(
        partial_out.astype(jnp.bfloat16).reshape(experts, capacity, partial_out.shape[1]), True, 3
    ).reshape(experts * capacity, middle.shape[1])
    result = middle.astype(jnp.float32)
    for k in range(top_count):
        chosen = (target[:, k][:, None] == slots[None, :]).astype(jnp.bfloat16)
        picked = jnp.dot(chosen, returned, preferred_element_type=jnp.float32)
        result = result + picked * expert_weights[:, k][:, None]
    return result.astype(jnp.bfloat16)


def solution(mesh):
    in_specs = (
        P("sp", "tp"),
        P("sp", "tp"),
        P("sp", "tp"),
        P("sp", "tp"),
        P("sp"),
        P("tp", None),
        P("sp", "tp"),
        P(),
        P("sp", None),
        P("sp", None),
        P("sp", None, "tp"),
        P("sp", None, "tp"),
        P("sp", "tp", None),
    )
    out_specs = P("sp", "tp")
    return jax.shard_map(shards, mesh=mesh, in_specs=in_specs, out_specs=out_specs, check_vma=False)
```

```python
import functools

import jax
import jax.numpy as jnp
from jax import lax
from jax.experimental import pallas as pl
from jax.experimental.pallas import tpu as pltpu
from jax.sharding import PartitionSpec as P

HEAD = 64
REACH = 4
LANES = 128
LOG2E = 1.4426950408889634

NORM_EPS = 1e-06
MESH = pl.DeviceIdType.MESH


def attention_kernel(
    count, q_ref, qdoc_ref, kv_ref, aux_ref, out_ref,
    kv_buf, aux_buf, acc, total, kv_send, kv_recv, aux_send, aux_recv,
):
    me = lax.axis_index("sp")
    odd = lax.rem(me, 2)
    even = 1 - odd
    partner = me + 1 - 2 * odd
    pairs, rows, _ = kv_ref.shape

    barrier = pltpu.get_barrier_semaphore()
    pl.semaphore_signal(barrier, inc=1, device_id={"sp": partner}, device_id_type=MESH)

    @pl.when(me + 2 < count)
    def _():
        pl.semaphore_signal(barrier, inc=1, device_id={"sp": me + 2}, device_id_type=MESH)

    @pl.when(me >= 2)
    def _():
        pl.semaphore_signal(barrier, inc=1, device_id={"sp": me - 2}, device_id_type=MESH)

    peers = 1 + jnp.where(me + 2 < count, 1, 0) + jnp.where(me >= 2, 1, 0)
    pl.semaphore_wait(barrier, peers)

    def own(item):
        return kv_ref.at[item] if item < pairs else aux_ref

    def slot(item, distance):
        return kv_buf.at[distance - 1, item] if item < pairs else aux_buf.at[distance - 1]

    def remote(item, source, distance, kind, target):
        if item < pairs:
            send, recv = kv_send.at[kind, item], kv_recv.at[distance - 1, item]
        else:
            send, recv = aux_send.at[kind], aux_recv.at[distance - 1]
        return pltpu.make_async_remote_copy(
            src_ref=source, dst_ref=slot(item, distance), send_sem=send, recv_sem=recv,
            device_id={"sp": target}, device_id_type=MESH,
        )

    has_next = me + 2 < count
    copies = {
        "chain": (has_next, lambda i: remote(i, own(i), 2, 0, me + 2)),
        "chain2": (has_next & (me >= 2), lambda i: remote(i, slot(i, 2), 4, 1, me + 2)),
        "even1": (even == 1, lambda i: remote(i, own(i), 1, 2, partner)),
        "even3": ((even == 1) & (me >= 2), lambda i: remote(i, slot(i, 2), 3, 3, partner)),
        "odd1": ((odd == 1) & (me >= 2), lambda i: remote(i, slot(i, 2), 1, 2, partner)),
        "odd3": ((odd == 1) & (me >= 4), lambda i: remote(i, slot(i, 4), 3, 3, partner)),
    }

    def start(name, items):
        condition, make = copies[name]

        @pl.when(condition)
        def _():
            for item in items:
                make(item).start()

    def arrive(distance, items):
        @pl.when(me >= distance)
        def _():
            for item in items:
                remote(item, slot(item, distance), distance, 0, partner).wait_recv()

    lane = lax.broadcasted_iota(jnp.int32, (rows, LANES), 1)
    row_of = lax.broadcasted_iota(jnp.int32, (rows, rows), 0)
    col_of = lax.broadcasted_iota(jnp.int32, (rows, rows), 1)
    later = jnp.where(row_of >= col_of, 1.0, 0.0).astype(jnp.bfloat16)
    qdoc = qdoc_ref[...]
    per_pair = LANES // HEAD

    def block(head, pair, half, distance, key_value, aux, aux_row):
        in_head = (lane >= half * HEAD) & (lane < (half + 1) * HEAD)
        cols = pl.ds(pair * LANES, LANES)
        query = q_ref[:, cols]
        query = jnp.where(in_head, query, jnp.zeros_like(query))
        scores = lax.dot_general(
            query, key_value[:, :LANES], (((1,), (1,)), ((), ())),
            preferred_element_type=jnp.float32,
        )
        scores = (scores * (HEAD ** -0.5) + aux_row(head)) * LOG2E
        admitted = qdoc == aux_row(aux.shape[0] - 1)
        if distance == 0:
            admitted = admitted & (col_of < row_of)
        rest = jnp.minimum(-scores, 0.0) - jnp.log2(1.0 + jnp.exp2(-jnp.abs(scores)))
        rest = jnp.where(admitted, rest, 0.0)
        high = rest.astype(jnp.bfloat16)
        low = (rest - high.astype(jnp.float32)).astype(jnp.bfloat16)
        suffix = jnp.dot(high, later, preferred_element_type=jnp.float32) + jnp.dot(
            low, later, preferred_element_type=jnp.float32
        )
        before = jnp.zeros((rows, 1), jnp.float32) if distance == 0 else total[head]
        weight = jnp.where(admitted, jnp.exp2(scores + suffix + before), 0.0).astype(jnp.bfloat16)
        product = jnp.dot(weight, key_value[:, LANES:], preferred_element_type=jnp.float32)
        product = jnp.where(in_head, product, 0.0)
        if distance == 0 and half == 0:
            acc[pair] = product
        else:
            acc[pair] += product
        total[head] = before + suffix[:, :1]

    def own_pair(pair):
        for half in range(per_pair):
            block(
                pair * per_pair + half, pair, half, 0, kv_ref[pair], aux_ref,
                lambda r: aux_ref[pl.ds(r, 1), :],
            )

    def far_pair(pair, distance):
        @pl.when(me >= distance)
        def _():
            for half in range(per_pair):
                block(
                    pair * per_pair + half, pair, half, distance,
                    kv_buf[distance - 1, pair], aux_buf.at[distance - 1],
                    lambda r: aux_buf[distance - 1, pl.ds(r, 1), :],
                )

    everything = (pairs,) + tuple(range(pairs))
    start("chain", everything)
    start("even1", everything)
    first, rest_items = (pairs, 0), tuple(range(1, pairs))
    own_pair(0)
    arrive(2, first)
    for name in ("chain2", "even3", "odd1"):
        start(name, first)
    for pair in range(1, pairs):
        own_pair(pair)
    arrive(2, rest_items)
    for name in ("chain2", "even3", "odd1"):
        start(name, rest_items)
    arrive(1, first)
    far_pair(0, 1)
    far_pair(0, 2)
    arrive(4, first)
    start("odd3", first)
    arrive(1, rest_items)
    for pair in range(1, pairs):
        far_pair(pair, 1)
        far_pair(pair, 2)
    arrive(4, rest_items)
    start("odd3", rest_items)
    arrive(3, first)
    far_pair(0, 3)
    far_pair(0, 4)
    arrive(3, rest_items)
    for pair in range(1, pairs):
        far_pair(pair, 3)
        far_pair(pair, 4)
    for pair in range(pairs):
        out_ref[:, pair * LANES:(pair + 1) * LANES] = acc[pair].astype(out_ref.dtype)
    for condition, make in copies.values():
        @pl.when(condition)
        def _(make=make):
            for item in everything:
                make(item).wait_send()


def attend(query_rows, key_rows, value_rows, key_shift, documents):
    count = lax.axis_size("sp")
    rows, width = query_rows.shape
    pairs = width // LANES
    key_value = jnp.stack([
        jnp.concatenate(
            [part[:, p * LANES:(p + 1) * LANES] for part in (key_rows, value_rows)], axis=1
        )
        for p in range(pairs)
    ])
    heads = key_shift.shape[1]
    docs = documents.astype(jnp.float32)
    aux = jnp.concatenate([
        jnp.transpose(key_shift).astype(jnp.float32),
        jnp.broadcast_to(docs[None, :], (8 - heads % 8, rows)),
    ])
    vmem = pl.BlockSpec(memory_space=pltpu.VMEM)
    return pl.pallas_call(
        functools.partial(attention_kernel, count),
        out_shape=jax.ShapeDtypeStruct((rows, width), jnp.bfloat16),
        in_specs=[vmem] * 4,
        out_specs=vmem,
        scratch_shapes=[
            pltpu.VMEM((REACH, pairs, rows, 2 * LANES), jnp.bfloat16),
            pltpu.VMEM((REACH,) + aux.shape, jnp.float32),
            pltpu.VMEM((pairs, rows, LANES), jnp.float32),
            pltpu.VMEM((heads, rows, 1), jnp.float32),
            pltpu.SemaphoreType.DMA((4, pairs)),
            pltpu.SemaphoreType.DMA((REACH, pairs)),
            pltpu.SemaphoreType.DMA((4,)),
            pltpu.SemaphoreType.DMA((REACH,)),
        ],
        compiler_params=pltpu.CompilerParams(collective_id=0, has_side_effects=True),
        name="attention",
    )(query_rows, docs[:, None], key_value, aux)


def greet(count, others):
    me = lax.axis_index("sp")
    barrier = pltpu.get_barrier_semaphore()

    def signal(r, carry):
        pl.semaphore_signal(
            barrier, inc=1, device_id={"sp": lax.rem(me + r, count)}, device_id_type=MESH
        )
        return carry

    if count > 1:
        lax.fori_loop(1, count, signal, 0)
    for other in others:
        pl.semaphore_signal(barrier, inc=1, device_id={"tp": other}, device_id_type=MESH)
    pl.semaphore_wait(barrier, count - 1 + len(others))


def each(low, high, body):
    def step(r, carry):
        body(r)
        return carry

    lax.fori_loop(low, high, step, 0)


def mate(me, r, count):
    assert count & (count - 1) == 0
    other, bit = 0, 1
    while bit < count:
        other = other + bit * lax.rem(lax.div(me, bit) + lax.div(r, bit), 2)
        bit *= 2
    return other


def neighbours():
    t = lax.axis_index("tp")
    return t, t + 1 - 2 * lax.rem(t, 2), lax.rem(t + 2, lax.axis_size("tp"))


def dispatch_kernel(count, in_ref, gain_ref, out_ref, held, send, recv):
    me = lax.axis_index("sp")
    t, partner, across = neighbours()
    _, capacity, feats = in_ref.shape
    features = held.shape[2]
    greet(count, (partner, across))

    def columns(owner):
        return pl.ds(pl.multiple_of(owner * feats, feats), feats)

    def source(r):
        return mate(me, jnp.int32(r), count)

    def arrival(r):
        target = source(r)
        return pltpu.make_async_remote_copy(
            src_ref=in_ref.at[target], dst_ref=held.at[me, :, columns(t)],
            send_sem=send.at[0, r], recv_sem=recv.at[0, r],
            device_id={"sp": target}, device_id_type=MESH,
        )

    def share(r, kind, owner, target):
        place = held.at[source(r), :, columns(owner)]
        return pltpu.make_async_remote_copy(
            src_ref=place, dst_ref=place, send_sem=send.at[kind, r], recv_sem=recv.at[kind, r],
            device_id={"tp": target}, device_id_type=MESH,
        )

    def cross(r):
        return share(r, 1, t, across)

    def pair(r):
        return share(r, 2, t, partner)

    def relay(r):
        return share(r, 3, across, partner)

    def spread(r):
        cross(r).start()
        pair(r).start()

    def norm(r):
        pair(r).wait_recv()
        relay(r).wait_recv()
        row_block = held[source(r)].astype(jnp.float32)
        square_mean = jnp.sum(row_block * row_block, axis=1, keepdims=True) / features
        out_ref[source(r)] = (
            row_block * lax.rsqrt(square_mean + NORM_EPS) * gain_ref[...]
        ).astype(out_ref.dtype)

    each(1, count, lambda r: arrival(r).start())
    local = pltpu.make_async_copy(in_ref.at[me], held.at[me, :, columns(t)], send.at[0, 0])
    local.start()
    local.wait()
    spread(0)

    def take(r):
        arrival(r).wait_recv()
        spread(r)

    each(1, count, take)

    def forward(r):
        cross(r).wait_recv()
        relay(r).start()

    forward(0)

    def finish(r):
        forward(r)
        norm(r - 1)

    each(1, count, finish)
    norm(count - 1)
    each(1, count, lambda r: arrival(r).wait_send())

    def drain(r):
        cross(r).wait_send()
        pair(r).wait_send()
        relay(r).wait_send()

    each(0, count, drain)


def reduce_kernel(count, back, in_ref, out_ref, near, outgoing, far, final, send, recv):
    me = lax.axis_index("sp")
    t, partner, across = neighbours()
    partner_across = lax.rem(partner + 2, lax.axis_size("tp"))
    blocks, rows, _ = in_ref.shape
    feats = out_ref.shape[2]
    greet(count if back else 1, (partner, across))

    def columns(owner):
        return pl.ds(pl.multiple_of(owner * feats, feats), feats)

    def place(r):
        return mate(me, jnp.int32(blocks - 1 - r), blocks) if back else r

    def pair(r, which, owner):
        return pltpu.make_async_remote_copy(
            src_ref=in_ref.at[place(r), :, columns(owner)], dst_ref=near.at[which, r],
            send_sem=send.at[which, r], recv_sem=recv.at[which, r],
            device_id={"tp": partner}, device_id_type=MESH,
        )

    def cross(r):
        return pltpu.make_async_remote_copy(
            src_ref=outgoing.at[r], dst_ref=far.at[r],
            send_sem=send.at[2, r], recv_sem=recv.at[2, r],
            device_id={"tp": across}, device_id_type=MESH,
        )

    def home(r):
        return pltpu.make_async_remote_copy(
            src_ref=final.at[r], dst_ref=out_ref.at[me],
            send_sem=send.at[3, r], recv_sem=recv.at[3, r],
            device_id={"sp": place(r)}, device_id_type=MESH,
        )

    def start_pair(r):
        pair(r, 0, partner_across).start()
        pair(r, 1, partner).start()

    each(0, blocks, start_pair)

    def halve(r):
        pair(r, 0, partner_across).wait_recv()
        outgoing[r] = (
            in_ref[place(r), :, columns(across)].astype(jnp.float32)
            + near[0, r].astype(jnp.float32)
        ).astype(outgoing.dtype)
        cross(r).start()

    each(0, blocks, halve)

    def total(r):
        pair(r, 1, partner).wait_recv()
        cross(r).wait_recv()
        return (
            in_ref[place(r), :, columns(t)].astype(jnp.float32)
            + near[1, r].astype(jnp.float32)
            + far[r].astype(jnp.float32)
        ).astype(out_ref.dtype)

    def drain(r):
        pair(r, 0, partner_across).wait_send()
        pair(r, 1, partner).wait_send()
        cross(r).wait_send()

    if back:
        def finish(r):
            final[r] = total(r)
            home(r).start()

        each(0, blocks - 1, finish)
        out_ref[me] = total(blocks - 1)

        def collect(r):
            home(r).wait_recv()
            home(r).wait_send()

        each(0, blocks - 1, collect)
    else:
        def finish(r):
            out_ref[r] = total(r)

        each(0, blocks, finish)
    each(0, blocks, drain)


def dispatch(blocks, norm_gain):
    count, capacity, feats = blocks.shape
    features = norm_gain.shape[0]
    vmem = pl.BlockSpec(memory_space=pltpu.VMEM)
    return pl.pallas_call(
        functools.partial(dispatch_kernel, count),
        out_shape=jax.ShapeDtypeStruct((count, capacity, features), jnp.bfloat16),
        in_specs=[vmem] * 2,
        out_specs=vmem,
        scratch_shapes=[
            pltpu.VMEM((count, capacity, features), jnp.bfloat16),
            pltpu.SemaphoreType.DMA((4, count)),
            pltpu.SemaphoreType.DMA((4, count)),
        ],
        compiler_params=pltpu.CompilerParams(collective_id=1, has_side_effects=True),
        name="dispatch",
    )(blocks, norm_gain[None, :])


def reduce_tp(partial, back, collective_id):
    blocks, rows, features = partial.shape
    feats = features // lax.axis_size("tp")
    vmem = pl.BlockSpec(memory_space=pltpu.VMEM)
    slots = pltpu.VMEM((blocks, rows, feats), jnp.bfloat16)
    return pl.pallas_call(
        functools.partial(reduce_kernel, lax.axis_size("sp"), back),
        out_shape=jax.ShapeDtypeStruct((blocks, rows, feats), jnp.bfloat16),
        in_specs=[vmem],
        out_specs=vmem,
        scratch_shapes=[
            pltpu.VMEM((2, blocks, rows, feats), jnp.bfloat16),
            slots,
            slots,
            slots if back else pltpu.VMEM((8, 128), jnp.bfloat16),
            pltpu.SemaphoreType.DMA((4, blocks)),
            pltpu.SemaphoreType.DMA((4, blocks)),
        ],
        compiler_params=pltpu.CompilerParams(collective_id=collective_id, has_side_effects=True),
        name="combine" if back else "project",
    )(partial)


def shards(
    query_rows,
    key_rows,
    value_rows,
    key_shift,
    documents,
    out_weight,
    stream,
    norm_gain,
    expert_ids,
    expert_weights,
    gate_weight,
    up_weight,
    down_weight,
):
    portion_rows = query_rows.shape[0]
    attended = attend(query_rows, key_rows, value_rows, key_shift, documents)
    partial_value = jnp.dot(attended, out_weight, preferred_element_type=jnp.float32).astype(
        jnp.bfloat16
    )
    cuts = 4 if portion_rows % 64 == 0 else 1
    projected = reduce_tp(
        partial_value.reshape(cuts, portion_rows // cuts, partial_value.shape[1]), False, 2
    ).reshape(portion_rows, stream.shape[1])
    middle = (stream.astype(jnp.float32) + projected.astype(jnp.float32)).astype(jnp.bfloat16)
    top_count = expert_ids.shape[1]
    experts = lax.axis_size("sp") * gate_weight.shape[0]
    capacity = (4 * portion_rows * top_count + 3 * experts - 1) // (3 * experts)
    capacity = (capacity + 15) // 16 * 16
    flat_ids = expert_ids.reshape(portion_rows * top_count)
    onehot = (flat_ids[:, None] == jnp.arange(experts, dtype=jnp.int32)[None, :]).astype(jnp.int32)
    slot_index = jnp.sum((jnp.cumsum(onehot, axis=0) - 1) * onehot, axis=1)
    target = (flat_ids * capacity + slot_index).reshape(portion_rows, top_count)
    slots = jnp.arange(experts * capacity, dtype=jnp.int32)
    placed = target[:, 0][None, :] == slots[:, None]
    for k in range(1, top_count):
        placed = placed | (target[:, k][None, :] == slots[:, None])
    blocks = jnp.dot(
        placed.astype(jnp.bfloat16), middle, preferred_element_type=jnp.float32
    ).astype(jnp.bfloat16)
    arrived = dispatch(blocks.reshape(experts, capacity, middle.shape[1]), norm_gain)
    row_block = arrived.reshape(experts * capacity, arrived.shape[2])
    gate_value = jnp.dot(row_block, gate_weight[0], preferred_element_type=jnp.float32)
    up_value = jnp.dot(row_block, up_weight[0], preferred_element_type=jnp.float32)
    hidden = (jax.nn.silu(gate_value) * up_value).astype(jnp.bfloat16)
    partial_out = jnp.dot(hidden, down_weight[0], preferred_element_type=jnp.float32)
    returned = reduce_tp(
        partial_out.astype(jnp.bfloat16).reshape(experts, capacity, partial_out.shape[1]), True, 3
    ).reshape(experts * capacity, middle.shape[1])
    result = middle.astype(jnp.float32)
    for k in range(top_count):
        chosen = (target[:, k][:, None] == slots[None, :]).astype(jnp.bfloat16)
        picked = jnp.dot(chosen, returned, preferred_element_type=jnp.float32)
        result = result + picked * expert_weights[:, k][:, None]
    return result.astype(jnp.bfloat16)


def solution(mesh):
    in_specs = (
        P("sp", "tp"),
        P("sp", "tp"),
        P("sp", "tp"),
        P("sp", "tp"),
        P("sp"),
        P("tp", None),
        P("sp", "tp"),
        P(),
        P("sp", None),
        P("sp", None),
        P("sp", None, "tp"),
        P("sp", None, "tp"),
        P("sp", "tp", None),
    )
    out_specs = P("sp", "tp")
    return jax.shard_map(shards, mesh=mesh, in_specs=in_specs, out_specs=out_specs, check_vma=False)
```
